32 devices in a mesh: sp: 4 (over z), tp: 4 (over y, x), dp: 2 (over core).
Axes of the slice: x: 2, y: 2, z: 4, core: 2. Of those that a mesh axis runs over, the one named last changes fastest.
Arguments:
- latent: bfloat16 [4, 4096, 2048], P('dp', 'sp'), may hold values from -6 to 6
- context: bfloat16 [4, 1024, 2048], P('dp', 'sp'), may hold values from -6 to 6
- condition: bfloat16 [4, 2048], P('dp', 'sp'), may hold values from -6 to 6
- ctx_cond: bfloat16 [2048], P('sp'), may hold values from -6 to 6
- norm_gain: float32 [2048], replicated, may hold values from 0.1 to 1.9
- w_shift: bfloat16 [2048, 2048], P('sp', 'tp'), may hold values from -0.125 to 0.125
- w_scale: bfloat16 [2048, 2048], P('sp', 'tp'), may hold values from -0.125 to 0.125
- w_gate: bfloat16 [2048, 2048], P('sp', 'tp'), may hold values from -0.125 to 0.125
- w_query: bfloat16 [2048, 1024], P(None, 'tp'), may hold values from -0.125 to 0.125
- w_key: bfloat16 [2048, 256], P(None, 'tp'), may hold values from -0.125 to 0.125
- w_value: bfloat16 [2048, 256], P(None, 'tp'), may hold values from -0.125 to 0.125
- w_out: bfloat16 [1024, 2048], P('tp'), may hold values from -4 to 4
- sink_logit: float32 [16], P('tp'), may hold values from 4 to 7
- ctx_lift: float32 [16], P('tp'), may hold values from -4 to 220
Outputs:
- mixed: bfloat16 [4, 4096, 2048], P('dp', ('sp', 'tp'))
The draws below stay inside these ranges and needn't reach their ends.
All inputs are finite; a program needn't handle non-finite values.
Results may differ from the reference program's by a relative error of at most 0.012.
Values may be sent and summed in bfloat16 or wider, within the bound.
No kernel may reach another device: no remote copies, remote signals or barrier semaphores. Data moves between devices by JAX's collectives and lax.ppermute only.
A program may use at most 128 MiB of HBM per device.

```python
import jax
import jax.numpy as jnp
from jax import lax

D = 2048
HEADS = 16
KV_HEADS = 4
HEAD = 64
WINDOW = 128
GRID_COLS = 64
TOK_DEV = 1024
CTX = 1024
SAMPLES = 4
LATENT = 4096


def draw_ctx_lift(key, part):
    first_key = jax.random.fold_in(key, 11)
    lifted = jax.random.uniform(first_key, (HEADS,), jnp.float32, -3.6, -1.8)
    return lifted


def level_of(own_key, dims, cuts, smallest, largest):
    factor_of = 1.0
    for position, blocks in cuts:
        steps = jax.random.uniform(jax.random.fold_in(jax.random.fold_in(own_key, 6), position), (blocks,), jnp.float32, smallest / len(cuts), largest / len(cuts))
        factor_of = factor_of * jnp.repeat(jnp.exp(steps), dims[position] // blocks).reshape((-1,) + (1,) * (len(dims) - 1 - position))
    return factor_of


def centred(stream_key, shape, deviation, limit, cuts=(), kind=jnp.bfloat16):
    level = level_of(stream_key, shape, cuts, -0.22, 0.18) if cuts else 1.0
    array = jax.random.normal(stream_key, shape, jnp.float32) * deviation * level
    return jnp.minimum(jnp.maximum(array, -limit), limit).astype(kind)


def setup_inputs(seed: int = 0) -> dict:
    splits = jax.random.split(jax.random.key(seed), 15)
    return {
        "latent": centred(splits[0], (SAMPLES, LATENT, D), 1.0, 6.0, ((0, 2), (1, 4))),
        "context": centred(splits[1], (SAMPLES, CTX, D), 1.0, 6.0, ((0, 2), (1, 4))),
        "condition": centred(splits[2], (SAMPLES, D), 1.0, 6.0, ((0, 2), (1, 4))),
        "ctx_cond": centred(splits[3], (D,), 1.0, 6.0, ((0, 4),)),
        "norm_gain": jnp.clip(1.0 + 0.18 * jax.random.normal(splits[4], (D,), jnp.float32), 0.1, 1.9),
        "w_shift": centred(splits[5], (D, D), D ** -0.5, 0.125, ((0, 4), (1, 4))),
        "w_scale": centred(splits[6], (D, D), D ** -0.5, 0.125, ((0, 4), (1, 4))),
        "w_gate": centred(splits[7], (D, D), D ** -0.5, 0.125, ((0, 4), (1, 4))),
        "w_query": centred(splits[8], (D, HEADS * HEAD), D ** -0.5, 0.125, ((1, 4),)),
        "w_key": centred(splits[9], (D, KV_HEADS * HEAD), D ** -0.5, 0.125, ((1, 4),)),
        "w_value": centred(splits[10], (D, KV_HEADS * HEAD), D ** -0.5, 0.125, ((1, 4),)),
        "w_out": centred(splits[11], (HEADS * HEAD, D), 2 ** -0.5, 4.0, ((0, 4),)),
        "sink_logit": jnp.clip(4.0 + 3.0 * jax.random.uniform(splits[12], (HEADS,), jnp.float32) ** level_of(splits[12], (HEADS,), ((0, 4),), -0.2, 0.2), 4.0, 7.0),
        "ctx_lift": draw_ctx_lift(jax.random.fold_in(splits[14], 71), 0),
    }


epsilon = 1e-06
rope_base = 10000.0
masked_value = -1e+30

def modulated(inputs, norm_gain, shift_vec, scale_vec):
    widened = inputs.astype(jnp.float32)
    inverse = lax.rsqrt(lax.optimization_barrier(jnp.mean(widened * widened, axis=-1, keepdims=True)) + epsilon)
    return (widened * inverse * norm_gain * (1.0 + scale_vec) + shift_vec).astype(jnp.bfloat16)

def rotate_half(half_part, angles):
    first_half, second = jnp.split(half_part, 2, axis=-1)
    cosine = jnp.cos(angles)[:, None, :]
    sine_part = jnp.sin(angles)[:, None, :]
    return jnp.concatenate([first_half * cosine - second * sine_part, first_half * sine_part + second * cosine], axis=-1)

def rotate(inputs, positions):
    quarter = inputs.shape[-1] // 4
    frequency = rope_base ** (-jnp.arange(quarter, dtype=jnp.float32) / quarter)
    row_angle = (positions // GRID_COLS).astype(jnp.float32)[:, None] * frequency
    col_angle = (positions % GRID_COLS).astype(jnp.float32)[:, None] * frequency
    half_size = 2 * quarter
    return jnp.concatenate([rotate_half(inputs[..., :half_size], row_angle), rotate_half(inputs[..., half_size:], col_angle)], axis=-1)

def reference(latent, context, condition, ctx_cond, norm_gain, w_shift, w_scale, w_gate, w_query, w_key, w_value, w_out, sink_logit, ctx_lift):
    samples, latent_len, model_width = latent.shape
    cond_rows = jnp.concatenate([condition, ctx_cond[None, :]], axis=0)
    active = jax.nn.silu(cond_rows.astype(jnp.float32)).astype(jnp.bfloat16)
    shift_vec = jnp.dot(active, w_shift, preferred_element_type=jnp.float32)
    scale_vec = jnp.dot(active, w_scale, preferred_element_type=jnp.float32)
    gate_vec = jnp.dot(active, w_gate, preferred_element_type=jnp.float32)
    hidden = modulated(latent, norm_gain, shift_vec[:samples, None, :], scale_vec[:samples, None, :])
    ctx_hidden = modulated(context, norm_gain, shift_vec[samples], scale_vec[samples])
    positions = jnp.arange(latent_len, dtype=jnp.int32)
    flat = hidden.reshape(-1, model_width)
    queries = rotate(jnp.dot(flat, w_query, preferred_element_type=jnp.float32).reshape(samples, latent_len, HEADS, HEAD), positions).astype(jnp.bfloat16)
    key_rows = rotate(jnp.dot(flat, w_key, preferred_element_type=jnp.float32).reshape(samples, latent_len, KV_HEADS, HEAD), positions).astype(jnp.bfloat16)
    values = jnp.dot(flat, w_value, preferred_element_type=jnp.float32).astype(jnp.bfloat16).reshape(samples, latent_len, KV_HEADS, HEAD)
    ctx_flat = ctx_hidden.reshape(-1, model_width)
    ctx_keys = jnp.dot(ctx_flat, w_key, preferred_element_type=jnp.float32).astype(jnp.bfloat16).reshape(samples, CTX, KV_HEADS, HEAD)
    ctx_values = jnp.dot(ctx_flat, w_value, preferred_element_type=jnp.float32).astype(jnp.bfloat16).reshape(samples, CTX, KV_HEADS, HEAD)
    padding = ((0, 0), (WINDOW, WINDOW), (0, 0), (0, 0))
    key_pad = jnp.pad(key_rows, padding)
    value_pad = jnp.pad(values, padding)
    block_rows = min(512, TOK_DEV)
    blocks = latent_len // block_rows
    span_rows = block_rows + 2 * WINDOW
    group_size = HEADS // KV_HEADS
    lift_rows = ctx_lift.astype(jnp.float32).reshape(KV_HEADS, group_size, 1, 1)
    sink_rows = sink_logit.astype(jnp.float32).reshape(KV_HEADS, group_size, 1, 1)
    factor = HEAD ** (-0.5)

    def attend(step_id):
        sample = step_id // blocks
        row_start = step_id % blocks * block_rows
        q_rows = lax.dynamic_slice_in_dim(lax.dynamic_index_in_dim(queries, sample, 0, keepdims=False), row_start, block_rows, 0)
        q_rows = q_rows.reshape(block_rows, KV_HEADS, group_size, HEAD).astype(jnp.float32)
        near_keys = lax.dynamic_slice_in_dim(lax.dynamic_index_in_dim(key_pad, sample, 0, keepdims=False), row_start, span_rows, 0).astype(jnp.float32)
        near_values = lax.dynamic_slice_in_dim(lax.dynamic_index_in_dim(value_pad, sample, 0, keepdims=False), row_start, span_rows, 0).astype(jnp.float32)
        far_keys = lax.dynamic_index_in_dim(ctx_keys, sample, 0, keepdims=False).astype(jnp.float32)
        far_values = lax.dynamic_index_in_dim(ctx_values, sample, 0, keepdims=False).astype(jnp.float32)
        query_pos = row_start + jnp.arange(block_rows, dtype=jnp.int32)
        key_pos = row_start - WINDOW + jnp.arange(span_rows, dtype=jnp.int32)
        inside = (key_pos[None, :] >= 0) & (key_pos[None, :] < latent_len) & (jnp.abs(query_pos[:, None] - key_pos[None, :]) <= WINDOW)
        near_scores = jnp.einsum('qgrd,kgd->grqk', q_rows, near_keys) * factor
        near_scores = jnp.where(inside[None, None], near_scores, masked_value)
        far_scores = jnp.einsum('qgrd,kgd->grqk', q_rows, far_keys) * factor + lift_rows
        row_max = jnp.maximum(jnp.maximum(near_scores.max(-1, keepdims=True), far_scores.max(-1, keepdims=True)), sink_rows)
        near_exp = jnp.exp(near_scores - row_max)
        far_exp = jnp.exp(far_scores - row_max)
        normaliser = near_exp.sum(-1, keepdims=True) + far_exp.sum(-1, keepdims=True) + jnp.exp(sink_rows - row_max)
        near_weights = (near_exp / normaliser).astype(jnp.bfloat16).astype(jnp.float32)
        far_weights = (far_exp / normaliser).astype(jnp.bfloat16).astype(jnp.float32)
        outcome = jnp.einsum('grqk,kgd->qgrd', near_weights, near_values) + jnp.einsum('grqk,kgd->qgrd', far_weights, far_values)
        return outcome.astype(jnp.bfloat16).reshape(block_rows, HEADS * HEAD)
    attended = lax.map(attend, jnp.arange(samples * blocks, dtype=jnp.int32)).reshape(samples, latent_len, HEADS * HEAD)
    projected = jnp.dot(attended.reshape(-1, HEADS * HEAD), w_out, preferred_element_type=jnp.float32).reshape(samples, latent_len, model_width)
    return (gate_vec[:samples, None, :] * projected).astype(jnp.bfloat16)
```

```python
import functools

import jax
import jax.numpy as jnp
from jax import lax
from jax.experimental import pallas as pl
from jax.experimental.pallas import tpu as pltpu
from jax.sharding import PartitionSpec as P

HEAD = 64
WINDOW = 128
GRID_COLS = 64
LANES = 128

epsilon = 1e-06
rope_base = 10000.0
masked_value = -1e30
LOG2E = 1.4426950408889634
DIRECT = 4

f32 = jnp.float32
bf16 = jnp.bfloat16


def shifted(piece, axis, hop):
    count = lax.axis_size(axis)
    return lax.ppermute(piece, axis, [(i, (i + hop) % count) for i in range(count)])


def mod_kernel(cond_ref, shift_ref, scale_ref, gate_ref, out_ref):
    rows = cond_ref[...].astype(f32)
    active = (rows / (1.0 + jnp.exp(-rows))).astype(bf16)
    width = shift_ref.shape[1]
    for slot, weight in enumerate((shift_ref, scale_ref, gate_ref)):
        out_ref[:, slot * width : (slot + 1) * width] = jnp.dot(
            active, weight[...], preferred_element_type=f32
        )


def modulation(condition, ctx_cond, w_shift, w_scale, w_gate):
    rows = jnp.concatenate([condition, ctx_cond[None, :]], axis=0)
    part = pl.pallas_call(
        mod_kernel,
        out_shape=jax.ShapeDtypeStruct((rows.shape[0], 3 * w_shift.shape[1]), f32),
        name="mod_part",
    )(rows, w_shift, w_scale, w_gate)
    sp_count = lax.axis_size("sp")
    tp_count = lax.axis_size("tp")
    if sp_count <= DIRECT:
        pieces = [part] + [shifted(part, "sp", hop) for hop in range(1, sp_count)]
        part = functools.reduce(lambda a, b: a + b, pieces)
    else:
        part = lax.psum(part, "sp")
    part = part.reshape(rows.shape[0], 3, -1)
    width = part.shape[2]
    if tp_count <= DIRECT:
        mine = lax.axis_index("tp")
        full = jnp.zeros(part.shape[:2] + (width * tp_count,), f32)
        for hop in range(tp_count):
            piece = shifted(part, "tp", hop) if hop else part
            full = lax.dynamic_update_slice_in_dim(
                full, piece, ((mine - hop) % tp_count) * width, 2
            )
    else:
        full = lax.all_gather(part, "tp", axis=2, tiled=True)
    return full


def normed(rows, gain_row, shift_row):
    widened = rows.astype(f32)
    inverse = lax.rsqrt(jnp.mean(widened * widened, axis=-1, keepdims=True) + epsilon)
    return (widened * inverse * gain_row + shift_row).astype(bf16)


def ctx_kernel(x_ref, gain_ref, shift_ref, wk_ref, wv_ref, out_ref, w_scr):
    @pl.when(pl.program_id(0) == 0)
    def _():
        w_scr[:, :HEAD] = wk_ref[...]
        w_scr[:, HEAD:] = wv_ref[...]

    hidden = normed(x_ref[0], gain_ref[...], shift_ref[...])
    out_ref[0] = jnp.dot(hidden, w_scr[...], preferred_element_type=f32).astype(bf16)


def ctx_pairs(context, gain_row, shift_row, w_key, w_value):
    samples, rows, width = context.shape
    return pl.pallas_call(
        ctx_kernel,
        grid=(samples,),
        in_specs=[
            pl.BlockSpec((1, rows, width), lambda s: (s, 0, 0)),
            pl.BlockSpec((1, width), lambda s: (0, 0)),
            pl.BlockSpec((1, width), lambda s: (0, 0)),
            pl.BlockSpec(w_key.shape, lambda s: (0, 0)),
            pl.BlockSpec(w_value.shape, lambda s: (0, 0)),
        ],
        out_specs=pl.BlockSpec((1, rows, 2 * HEAD), lambda s: (s, 0, 0)),
        out_shape=jax.ShapeDtypeStruct((samples, rows, 2 * HEAD), bf16),
        scratch_shapes=[pltpu.VMEM((width, 2 * HEAD), bf16)],
        name="ctx_proj",
    )(context, gain_row, shift_row, w_key, w_value)


def proj_kernel(
    x_ref, gain_ref, shift_ref, wq_ref, wk_ref, wv_ref, cos_ref, lo_ref, hi_ref,
    q_ref, kv_ref, w_scr,
):
    cols = wq_ref.shape[1]

    @pl.when(pl.program_id(0) == 0)
    def _():
        w_scr[:, :cols] = wq_ref[...]
        w_scr[:, cols : cols + HEAD] = wk_ref[...]
        w_scr[:, cols + HEAD :] = wv_ref[...]

    hidden = normed(x_ref[0], gain_ref[...], shift_ref[...])
    product = jnp.dot(hidden, w_scr[...], preferred_element_type=f32)
    cosine, low, high = cos_ref[...], lo_ref[...], hi_ref[...]

    def rotated(part):
        return (
            part * cosine
            + pltpu.roll(part, LANES - HEAD // 4, 1) * low
            + pltpu.roll(part, HEAD // 4, 1) * high
        )

    for start in range(0, cols, LANES):
        part = product[:, start : start + LANES]
        q_ref[:, start : start + LANES] = (rotated(part) * (LOG2E * HEAD**-0.5)).astype(bf16)
    part = product[:, cols:]
    lane = lax.broadcasted_iota(jnp.int32, part.shape, 1)
    kv_ref[...] = jnp.where(lane < HEAD, rotated(part), part).astype(bf16)


def projected_rows(latent, sample, gain_row, shift_row, w_query, w_key, w_value, tables):
    _, tokens, width = latent.shape
    block = min(256, tokens)
    cols = w_query.shape[1]
    table = pl.BlockSpec((block, LANES), lambda t: (t, 0))
    return pl.pallas_call(
        proj_kernel,
        grid=(tokens // block,),
        in_specs=[
            pl.BlockSpec((1, block, width), lambda t: (sample, t, 0)),
            pl.BlockSpec((1, width), lambda t: (0, 0)),
            pl.BlockSpec((1, width), lambda t: (0, 0)),
            pl.BlockSpec(w_query.shape, lambda t: (0, 0)),
            pl.BlockSpec(w_key.shape, lambda t: (0, 0)),
            pl.BlockSpec(w_value.shape, lambda t: (0, 0)),
            table,
            table,
            table,
        ],
        out_specs=[
            pl.BlockSpec((block, cols), lambda t: (t, 0)),
            pl.BlockSpec((block, 2 * HEAD), lambda t: (t, 0)),
        ],
        out_shape=[
            jax.ShapeDtypeStruct((tokens, cols), bf16),
            jax.ShapeDtypeStruct((tokens, 2 * HEAD), bf16),
        ],
        scratch_shapes=[pltpu.VMEM((width, cols + 2 * HEAD), bf16)],
        name="latent_proj",
    )(latent, gain_row, shift_row, w_query, w_key, w_value, *tables)


def rope_tables(tokens, offset):
    quarter = HEAD // 4
    positions = offset + jnp.arange(tokens, dtype=jnp.int32)
    frequency = rope_base ** (-jnp.arange(quarter, dtype=f32) / quarter)
    row_angle = (positions // GRID_COLS).astype(f32)[:, None] * frequency
    col_angle = (positions % GRID_COLS).astype(f32)[:, None] * frequency
    angles = jnp.concatenate([row_angle, col_angle], axis=1)
    cosine, sine = jnp.cos(angles), jnp.sin(angles)
    none = jnp.zeros((tokens, quarter), f32)
    c_row, c_col = cosine[:, :quarter], cosine[:, quarter:]
    s_row, s_col = sine[:, :quarter], sine[:, quarter:]
    twice = LANES // HEAD
    return (
        jnp.concatenate([c_row, c_row, c_col, c_col] * twice, axis=1),
        jnp.concatenate([-s_row, none, -s_col, none] * twice, axis=1),
        jnp.concatenate([none, s_row, none, s_col] * twice, axis=1),
    )


def attend_kernel(place_ref, lift_ref, sink_ref, q_ref, kv_ref, left_ref, right_ref, *rest, pieces, last_place):
    ctx_refs = rest[:pieces]
    out_ref, near_scr, nearv_scr, ctx_scr, ctxv_scr = rest[pieces:]
    step = pl.program_id(0)
    tokens = kv_ref.shape[0]
    piece_rows = ctx_refs[0].shape[1]
    block = q_ref.shape[0]
    heads = q_ref.shape[1] // HEAD

    @pl.when(step == 0)
    def _():
        near_scr[:WINDOW] = left_ref[...]
        near_scr[WINDOW : WINDOW + tokens] = kv_ref[...]
        near_scr[WINDOW + tokens :] = right_ref[...]
        for number, ref in enumerate(ctx_refs):
            ctx_scr[number * piece_rows : (number + 1) * piece_rows] = ref[0]
        for source, target in ((near_scr, nearv_scr), (ctx_scr, ctxv_scr)):
            turned = pltpu.roll(source[...].astype(f32), HEAD, 1)
            lane = lax.broadcasted_iota(jnp.int32, turned.shape, 1)
            target[...] = jnp.where(lane < HEAD, turned, 1.0).astype(bf16)

    ctx_rows, ctx_values = ctx_scr[...], ctxv_scr[...]
    row = lax.broadcasted_iota(jnp.int32, (WINDOW, WINDOW), 0)
    col = lax.broadcasted_iota(jnp.int32, (WINDOW, WINDOW), 1)
    contract = (((1,), (1,)), ((), ()))
    for sub in range(block // WINDOW):
        start = pl.multiple_of(step * block + sub * WINDOW, WINDOW)
        near_rows = near_scr[pl.ds(start, 3 * WINDOW), :]
        near_values = nearv_scr[pl.ds(start, 3 * WINDOW), :]
        left_from = jnp.where((place_ref[0] == 0) & (start == 0), 2 * WINDOW, 0)
        right_from = jnp.where(
            (place_ref[0] == last_place) & (start + WINDOW == tokens), 2 * WINDOW, 0
        )
        left_ok = col >= row + left_from
        right_ok = col + right_from <= row
        stacked = []
        lane = lax.broadcasted_iota(jnp.int32, (WINDOW, LANES), 1)
        for head in range(heads):
            chunk = q_ref[sub * WINDOW : (sub + 1) * WINDOW, head // 2 * LANES : head // 2 * LANES + LANES].astype(f32)
            if head % 2:
                chunk = pltpu.roll(chunk, HEAD, 1)
            stacked.append(jnp.where(lane < HEAD, chunk, 0.0).astype(bf16))
        stacked = jnp.concatenate(stacked, axis=0)
        far = lax.dot_general(stacked, ctx_rows, contract, preferred_element_type=f32)
        near = lax.dot_general(stacked, near_rows, contract, preferred_element_type=f32)
        outs = []
        for head in range(heads):
            span = slice(head * WINDOW, (head + 1) * WINDOW)
            lift = lift_ref[head] * LOG2E
            sink = sink_ref[head] * LOG2E
            far_h = far[span]
            near_h = near[span]
            near_l = jnp.where(left_ok, near_h[:, :WINDOW], masked_value)
            near_m = near_h[:, WINDOW : 2 * WINDOW]
            near_r = jnp.where(right_ok, near_h[:, 2 * WINDOW :], masked_value)
            near_max = jnp.maximum(jnp.maximum(near_l, near_m), near_r).max(-1, keepdims=True)
            top = jnp.maximum(
                jnp.maximum(near_max, far_h.max(-1, keepdims=True) + lift), sink
            )
            far_exp = jnp.exp2(far_h - (top - lift)).astype(bf16)
            near_exp = jnp.concatenate(
                [jnp.exp2(part - top).astype(bf16) for part in (near_l, near_m, near_r)], axis=1
            )
            acc = jnp.dot(far_exp, ctx_values, preferred_element_type=f32) + jnp.dot(
                near_exp, near_values, preferred_element_type=f32
            )
            total = pltpu.roll(acc, HEAD, 1) + jnp.exp2(sink - top)
            outs.append(acc / total)
        for pair in range(heads // 2):
            both = jnp.where(lane < HEAD, outs[2 * pair], pltpu.roll(outs[2 * pair + 1], HEAD, 1))
            out_ref[0, sub * WINDOW : (sub + 1) * WINDOW, pair * LANES : (pair + 1) * LANES] = both.astype(bf16)


def attended_rows(place, lift, sink, queries, pairs, left, right, ctx_pieces, sample, tp_count):
    tokens, cols = queries.shape
    block = tokens // tp_count
    pieces = len(ctx_pieces)
    piece_rows = ctx_pieces[0].shape[1]
    whole = lambda t, *_: (0, 0)
    grid_spec = pltpu.PrefetchScalarGridSpec(
        num_scalar_prefetch=3,
        grid=(tp_count,),
        in_specs=[
            pl.BlockSpec((block, cols), lambda t, *_: (t, 0)),
            pl.BlockSpec(pairs.shape, whole),
            pl.BlockSpec(left.shape, whole),
            pl.BlockSpec(right.shape, whole),
        ]
        + [pl.BlockSpec((1, piece_rows, 2 * HEAD), lambda t, *_: (sample, 0, 0))] * pieces,
        out_specs=pl.BlockSpec(
            (1, block, cols), lambda t, place, *_: (lax.rem(t - place[1] + tp_count, tp_count), 0, 0)
        ),
        scratch_shapes=[
            pltpu.VMEM((tokens + 2 * WINDOW, 2 * HEAD), bf16),
            pltpu.VMEM((tokens + 2 * WINDOW, 2 * HEAD), bf16),
            pltpu.VMEM((pieces * piece_rows, 2 * HEAD), bf16),
            pltpu.VMEM((pieces * piece_rows, 2 * HEAD), bf16),
        ],
    )
    return pl.pallas_call(
        functools.partial(attend_kernel, pieces=pieces, last_place=lax.axis_size("sp") - 1),
        grid_spec=grid_spec,
        out_shape=jax.ShapeDtypeStruct((tp_count, block, cols), bf16),
        name="attend",
    )(place, lift, sink, queries, pairs, left, right, *ctx_pieces)


def out_kernel(place_ref, *refs, hops):
    gate_ref = refs[0]
    pieces = refs[1 : 1 + hops]
    own_w = refs[1 + hops]
    near_w = refs[2 + hops : 1 + 2 * hops]
    far_w = refs[1 + 2 * hops : 3 * hops]
    out_ref = refs[-1]
    acc = jnp.dot(pieces[0][0], own_w[...], preferred_element_type=f32)
    first = place_ref[2] == 0
    for hop in range(1, hops):
        rows = pieces[hop][0]
        half = rows.shape[1] // 2
        low, high = rows[:, :half].astype(f32), rows[:, half:].astype(f32)
        mine = jnp.where(first, low, high).astype(bf16)
        other = jnp.where(first, high, low).astype(bf16)
        acc += jnp.dot(mine, near_w[hop - 1][...], preferred_element_type=f32)
        acc += jnp.dot(other, far_w[hop - 1][...], preferred_element_type=f32)
    out_ref[0] = (gate_ref[...] * acc).astype(bf16)


def out_rows(place, gate_row, pieces, own_w, near_w, far_w, sample, samples, previous):
    hops = len(pieces)
    block, cols = pieces[0].shape[1:]
    width = own_w.shape[1]
    tile = min(512, width)
    specs = [pl.BlockSpec((1, tile), lambda n, *_: (0, n))]
    specs += [pl.BlockSpec((1, block, cols), lambda n, *_: (0, 0, 0))] * hops
    specs += [pl.BlockSpec((cols, tile), lambda n, *_: (0, n))]
    specs += [pl.BlockSpec((cols // 2, tile), lambda n, *_: (0, n))] * (2 * (hops - 1))
    args = [gate_row, *pieces, own_w, *near_w, *far_w]
    aliases = {}
    if previous is not None:
        specs.append(pl.BlockSpec(memory_space=pl.ANY))
        args.append(previous)
        aliases = {len(args): 0}
    return pl.pallas_call(
        functools.partial(out_kernel, hops=hops),
        grid_spec=pltpu.PrefetchScalarGridSpec(
            num_scalar_prefetch=1,
            grid=(width // tile,),
            in_specs=specs,
            out_specs=pl.BlockSpec((1, block, tile), lambda n, *_: (sample, 0, n)),
        ),
        out_shape=jax.ShapeDtypeStruct((samples, block, width), bf16),
        input_output_aliases=aliases,
        name="out_proj",
    )(place, *args)


def shards(
    latent,
    context,
    condition,
    ctx_cond,
    norm_gain,
    w_shift,
    w_scale,
    w_gate,
    w_query,
    w_key,
    w_value,
    w_out,
    sink_logit,
    ctx_lift,
):
    samples, tokens, model_width = latent.shape
    sp_count = lax.axis_size("sp")
    tp_count = lax.axis_size("tp")
    place = jnp.stack(
        [lax.axis_index("sp"), lax.axis_index("tp"), lax.axis_index("dp")]
    ).astype(jnp.int32)
    tables = rope_tables(tokens, lax.axis_index("sp") * tokens)
    vectors = modulation(condition, ctx_cond, w_shift, w_scale, w_gate)
    gain = norm_gain * (1.0 + vectors[:, 1])
    shift, gate = vectors[:, 0], vectors[:, 2]

    ctx_own = ctx_pairs(context, gain[samples][None], shift[samples][None], w_key, w_value)
    if sp_count <= DIRECT:
        ctx_pieces = [ctx_own] + [shifted(ctx_own, "sp", hop) for hop in range(1, sp_count)]
    else:
        ctx_pieces = [lax.all_gather(ctx_own, "sp", axis=1, tiled=True)]

    half = w_out.shape[0] // 2
    w_out_late, _ = lax.optimization_barrier((w_out, gain))
    w_half = lax.dynamic_slice_in_dim(w_out_late, lax.axis_index("dp") * half, half, 0)
    near_w = [shifted(w_half, "tp", hop) for hop in range(1, tp_count)]
    far_w = [shifted(piece, "dp", 1) for piece in near_w]

    rows = []
    for sample in range(samples):
        queries, pairs = projected_rows(
            latent, sample, gain[sample][None], shift[sample][None], w_query, w_key, w_value, tables
        )
        left = lax.ppermute(pairs[-WINDOW:], "sp", [(i, i + 1) for i in range(sp_count - 1)])
        right = lax.ppermute(pairs[:WINDOW], "sp", [(i + 1, i) for i in range(sp_count - 1)])
        rows.append((queries, pairs, left, right))
    arrived = []
    for sample in range(samples):
        queries, pairs, left, right = rows[sample]
        attended = attended_rows(
            place, ctx_lift, sink_logit, queries, pairs, left, right, ctx_pieces, sample, tp_count
        )
        arrived.append(
            [attended[:1]] + [shifted(attended[hop : hop + 1], "tp", hop) for hop in range(1, tp_count)]
        )
    mixed = None
    for sample in range(samples):
        mixed = out_rows(
            place, gate[sample][None], arrived[sample], w_out, near_w, far_w, sample, samples, mixed
        )
    return mixed


def solution(mesh):
    return jax.shard_map(
        shards,
        mesh=mesh,
        in_specs=(
            P("dp", "sp", None),
            P("dp", "sp", None),
            P("dp", "sp"),
            P("sp"),
            P(),
            P("sp", "tp"),
            P("sp", "tp"),
            P("sp", "tp"),
            P(None, "tp"),
            P(None, "tp"),
            P(None, "tp"),
            P("tp", None),
            P("tp"),
            P("tp"),
        ),
        out_specs=P("dp", ("sp", "tp"), None),
        check_vma=False,
    )
```

```python
import functools

import jax
import jax.numpy as jnp
from jax import lax
from jax.experimental import pallas as pl
from jax.experimental.pallas import tpu as pltpu
from jax.sharding import PartitionSpec as P

HEAD = 64
WINDOW = 128
GRID_COLS = 64
LANES = 128

epsilon = 1e-06
rope_base = 10000.0
masked_value = -1e30
LOG2E = 1.4426950408889634
DIRECT = 4

f32 = jnp.float32
bf16 = jnp.bfloat16


def shifted(piece, axis, hop):
    count = lax.axis_size(axis)
    return lax.ppermute(piece, axis, [(i, (i + hop) % count) for i in range(count)])


def mod_kernel(cond_ref, ctx_ref, shift_ref, scale_ref, gate_ref, out_ref, rows_scr):
    samples = cond_ref.shape[0]
    rows_scr[:samples] = cond_ref[...].astype(f32)
    rows_scr[samples:] = ctx_ref[...].astype(f32)
    rows = rows_scr[...]
    active = (rows / (1.0 + jnp.exp(-rows))).astype(bf16)
    width = shift_ref.shape[1]
    for slot, weight in enumerate((shift_ref, scale_ref, gate_ref)):
        out_ref[:, slot * width : (slot + 1) * width] = jnp.dot(
            active, weight[...], preferred_element_type=f32
        )


def finish_kernel(place_ref, norm_ref, *refs, hops):
    gain_ref, shift_ref, gate_ref, sum_scr = refs[-4:]
    parts = refs[:-4]
    total = parts[0][...]
    for part in parts[1:]:
        total = total + part[...]
    rows = total.shape[1]
    width = total.shape[2] // 3
    for hop in range(hops):
        owner = lax.rem(place_ref[1] - hop + hops, hops)
        at = pl.ds(pl.multiple_of(owner * width, LANES), width)
        for slot in range(3):
            sum_scr[slot * rows : (slot + 1) * rows, at] = total[hop, :, slot * width : (slot + 1) * width]
    values = sum_scr[...]
    for row in range(rows):
        shift_ref[row] = values[row : row + 1]
        gain_ref[row] = norm_ref[...] * (1.0 + values[rows + row : rows + row + 1])
        gate_ref[row] = values[2 * rows + row : 2 * rows + row + 1]


def modulation(place, condition, ctx_cond, norm_gain, w_shift, w_scale, w_gate):
    rows = condition.shape[0] + 1
    width = w_shift.shape[1]
    part = pl.pallas_call(
        mod_kernel,
        out_shape=jax.ShapeDtypeStruct((rows, 3 * width), f32),
        scratch_shapes=[pltpu.VMEM((rows, condition.shape[1]), f32)],
        name="mod_part",
    )(condition, ctx_cond[None, :], w_shift, w_scale, w_gate)
    sp_count = lax.axis_size("sp")
    tp_count = lax.axis_size("tp")
    gathered = jnp.stack([part] + [shifted(part, "tp", hop) for hop in range(1, tp_count)])
    if sp_count <= DIRECT:
        parts = [gathered] + [shifted(gathered, "sp", hop) for hop in range(1, sp_count)]
    else:
        parts = [lax.psum(gathered, "sp")]
    model_width = norm_gain.shape[0]
    vector = jax.ShapeDtypeStruct((rows, 1, model_width), f32)
    smem = pl.BlockSpec(memory_space=pltpu.SMEM)
    vmem = pl.BlockSpec(memory_space=pltpu.VMEM)
    gain, shift, gate = pl.pallas_call(
        functools.partial(finish_kernel, hops=tp_count),
        in_specs=[smem, vmem] + [vmem] * len(parts),
        out_shape=[vector] * 3,
        scratch_shapes=[pltpu.VMEM((3 * rows, model_width), f32)],
        name="finish",
    )(place, norm_gain[None, :], *parts)
    return gain, shift, gate, gathered


def normed(rows, gain_row, shift_row):
    widened = rows.astype(f32)
    inverse = lax.rsqrt(jnp.mean(widened * widened, axis=-1, keepdims=True) + epsilon)
    return (widened * inverse * gain_row + shift_row).astype(bf16)


def small_tables(tokens, offset):
    quarter = HEAD // 4
    lane = jnp.arange(LANES, dtype=jnp.int32)[None, :]
    frequency = rope_base ** (-(lane % quarter).astype(f32) / quarter)
    groups = tokens // GRID_COLS
    number = jnp.arange(groups + GRID_COLS, dtype=jnp.int32)[:, None]
    of_row = number < groups
    turn = jnp.where(of_row, number + offset // GRID_COLS, number - groups).astype(f32)
    angle = turn * frequency
    used = of_row == (lane % HEAD < HEAD // 2)
    sign = jnp.where(lane // quarter % 2 == 0, -1.0, 1.0)
    return jnp.where(used, jnp.cos(angle), 0.0), jnp.where(used, jnp.sin(angle) * sign, 0.0)


def rotation(cos_ref, sin_ref, group, count):
    groups = cos_ref.shape[0] - GRID_COLS

    def table(ref):
        rows = [ref[pl.ds(group + i, 1), :] + ref[groups:, :] for i in range(count)]
        return jnp.concatenate(rows, axis=0)

    return table(cos_ref), table(sin_ref)


def rotated(part, cosine, sine):
    quarter = HEAD // 4
    lane = lax.broadcasted_iota(jnp.int32, part.shape, 1)
    partner = jnp.where(
        lane // quarter % 2 == 0,
        pltpu.roll(part, LANES - quarter, 1),
        pltpu.roll(part, quarter, 1),
    )
    return part * cosine + partner * sine


def rotated_pairs(part, cosine, sine):
    lane = lax.broadcasted_iota(jnp.int32, part.shape, 1)
    return jnp.where(lane < HEAD, rotated(part, cosine, sine), part).astype(bf16)


def early_kernel(
    x_ref, head_ref, tail_ref, gain_ref, shift_ref, cgain_ref, cshift_ref, wk_ref, wv_ref,
    cos_ref, sin_ref, ctx_ref, next_ref, prev_ref, w_scr,
):
    @pl.when(pl.program_id(0) == 0)
    def _():
        w_scr[:, :HEAD] = wk_ref[...]
        w_scr[:, HEAD:] = wv_ref[...]

    weights = w_scr[...]
    rows = x_ref.shape[1]
    groups = cos_ref.shape[0] - GRID_COLS
    edge = WINDOW // GRID_COLS
    hidden = normed(x_ref[0], cgain_ref[0], cshift_ref[0])
    ctx = jnp.dot(hidden, weights, preferred_element_type=f32).astype(bf16)
    ctx_ref[0] = ctx
    next_ref[0, :rows] = ctx
    prev_ref[0, :rows] = ctx
    for source, target, group in ((head_ref, prev_ref, 0), (tail_ref, next_ref, groups - edge)):
        hidden = normed(source[0], gain_ref[0], shift_ref[0])
        part = jnp.dot(hidden, weights, preferred_element_type=f32)
        target[0, rows:] = rotated_pairs(part, *rotation(cos_ref, sin_ref, group, edge))


def early_pairs(context, latent, gain, shift, w_key, w_value, tables):
    samples, rows, width = context.shape
    last = latent.shape[1] // WINDOW - 1
    vec = pl.BlockSpec((1, 1, width), lambda s: (s, 0, 0))
    ctx_vec = pl.BlockSpec((1, 1, width), lambda s: (samples, 0, 0))
    whole = lambda s: (0, 0)
    sizes = (rows, rows + WINDOW, rows + WINDOW)
    work = samples * (rows + 2 * WINDOW) * width
    return pl.pallas_call(
        early_kernel,
        grid=(samples,),
        in_specs=[
            pl.BlockSpec((1, rows, width), lambda s: (s, 0, 0)),
            pl.BlockSpec((1, WINDOW, width), lambda s: (s, 0, 0)),
            pl.BlockSpec((1, WINDOW, width), lambda s: (s, last, 0)),
            vec,
            vec,
            ctx_vec,
            ctx_vec,
            pl.BlockSpec(w_key.shape, whole),
            pl.BlockSpec(w_value.shape, whole),
            pl.BlockSpec(tables[0].shape, whole),
            pl.BlockSpec(tables[1].shape, whole),
        ],
        out_specs=[pl.BlockSpec((1, size, 2 * HEAD), lambda s: (s, 0, 0)) for size in sizes],
        out_shape=[jax.ShapeDtypeStruct((samples, size, 2 * HEAD), bf16) for size in sizes],
        scratch_shapes=[pltpu.VMEM((width, 2 * HEAD), bf16)],
        cost_estimate=pl.CostEstimate(flops=work * 4 * HEAD, transcendentals=0, bytes_accessed=2 * work),
        name="early_proj",
    )(context, latent, latent, gain, shift, gain, shift, w_key, w_value, *tables)


def proj_kernel(
    x_ref, gain_ref, shift_ref, wq_ref, wk_ref, wv_ref, cos_ref, sin_ref, q_ref, kv_ref, w_scr
):
    cols = wq_ref.shape[1]

    @pl.when((pl.program_id(0) == 0) & (pl.program_id(1) == 0))
    def _():
        w_scr[:, :cols] = wq_ref[...]
        w_scr[:, cols : cols + HEAD] = wk_ref[...]
        w_scr[:, cols + HEAD :] = wv_ref[...]

    count = x_ref.shape[1] // GRID_COLS
    hidden = normed(x_ref[0], gain_ref[0], shift_ref[0])
    product = jnp.dot(hidden, w_scr[...], preferred_element_type=f32)
    cosine, sine = rotation(cos_ref, sin_ref, pl.program_id(1) * count, count)
    for start in range(0, cols, LANES):
        part = rotated(product[:, start : start + LANES], cosine, sine)
        q_ref[0, :, start : start + LANES] = (part * (LOG2E * HEAD**-0.5)).astype(bf16)
    kv_ref[0] = rotated_pairs(product[:, cols:], cosine, sine)


def projected_rows(latent, gain, shift, w_query, w_key, w_value, tables):
    samples, tokens, width = latent.shape
    block = min(256, tokens)
    cols = w_query.shape[1]
    vec = pl.BlockSpec((1, 1, width), lambda s, t: (s, 0, 0))
    whole = lambda s, t: (0, 0)
    work = samples * tokens * width
    return pl.pallas_call(
        proj_kernel,
        grid=(samples, tokens // block),
        in_specs=[
            pl.BlockSpec((1, block, width), lambda s, t: (s, t, 0)),
            vec,
            vec,
            pl.BlockSpec(w_query.shape, whole),
            pl.BlockSpec(w_key.shape, whole),
            pl.BlockSpec(w_value.shape, whole),
            pl.BlockSpec(tables[0].shape, whole),
            pl.BlockSpec(tables[1].shape, whole),
        ],
        out_specs=[
            pl.BlockSpec((1, block, cols), lambda s, t: (s, t, 0)),
            pl.BlockSpec((1, block, 2 * HEAD), lambda s, t: (s, t, 0)),
        ],
        out_shape=[
            jax.ShapeDtypeStruct((samples, tokens, cols), bf16),
            jax.ShapeDtypeStruct((samples, tokens, 2 * HEAD), bf16),
        ],
        scratch_shapes=[pltpu.VMEM((width, cols + 2 * HEAD), bf16)],
        cost_estimate=pl.CostEstimate(
            flops=work * 2 * (cols + 2 * HEAD), transcendentals=0, bytes_accessed=2 * work
        ),
        name="latent_proj",
    )(latent, gain, shift, w_query, w_key, w_value, *tables)


def attend_kernel(place_ref, lift_ref, sink_ref, q_ref, kv_ref, left_ref, right_ref, *rest, pieces, last_place):
    ctx_refs = rest[:pieces]
    out_ref, near_scr, nearv_scr, ctx_scr, ctxv_scr = rest[pieces:]
    step = pl.program_id(0)
    tokens = kv_ref.shape[1]
    piece_rows = ctx_scr.shape[0] // pieces
    block = q_ref.shape[1]
    heads = q_ref.shape[2] // HEAD

    @pl.when(step == 0)
    def _():
        near_scr[:WINDOW] = left_ref[0, left_ref.shape[1] - WINDOW :]
        near_scr[WINDOW : WINDOW + tokens] = kv_ref[0]
        near_scr[WINDOW + tokens :] = right_ref[0, right_ref.shape[1] - WINDOW :]
        for number, ref in enumerate(ctx_refs):
            ctx_scr[number * piece_rows : (number + 1) * piece_rows] = ref[0, :piece_rows]
        for source, target in ((near_scr, nearv_scr), (ctx_scr, ctxv_scr)):
            turned = pltpu.roll(source[...].astype(f32), HEAD, 1)
            lane = lax.broadcasted_iota(jnp.int32, turned.shape, 1)
            target[...] = jnp.where(lane < HEAD, turned, 1.0).astype(bf16)

    ctx_rows, ctx_values = ctx_scr[...], ctxv_scr[...]
    row = lax.broadcasted_iota(jnp.int32, (WINDOW, WINDOW), 0)
    col = lax.broadcasted_iota(jnp.int32, (WINDOW, WINDOW), 1)
    contract = (((1,), (1,)), ((), ()))
    for sub in range(block // WINDOW):
        start = pl.multiple_of(step * block + sub * WINDOW, WINDOW)
        near_rows = near_scr[pl.ds(start, 3 * WINDOW), :]
        near_values = nearv_scr[pl.ds(start, 3 * WINDOW), :]
        left_from = jnp.where((place_ref[0] == 0) & (start == 0), 2 * WINDOW, 0)
        right_from = jnp.where(
            (place_ref[0] == last_place) & (start + WINDOW == tokens), 2 * WINDOW, 0
        )
        left_ok = col >= row + left_from
        right_ok = col + right_from <= row
        stacked = []
        lane = lax.broadcasted_iota(jnp.int32, (WINDOW, LANES), 1)
        for head in range(heads):
            chunk = q_ref[0, sub * WINDOW : (sub + 1) * WINDOW, head // 2 * LANES : head // 2 * LANES + LANES].astype(f32)
            if head % 2:
                chunk = pltpu.roll(chunk, HEAD, 1)
            stacked.append(jnp.where(lane < HEAD, chunk, 0.0).astype(bf16))
        stacked = jnp.concatenate(stacked, axis=0)
        far = lax.dot_general(stacked, ctx_rows, contract, preferred_element_type=f32)
        near = lax.dot_general(stacked, near_rows, contract, preferred_element_type=f32)
        outs = []
        for head in range(heads):
            span = slice(head * WINDOW, (head + 1) * WINDOW)
            lift = lift_ref[head] * LOG2E
            sink = sink_ref[head] * LOG2E
            far_h = far[span]
            near_h = near[span]
            near_l = jnp.where(left_ok, near_h[:, :WINDOW], masked_value)
            near_m = near_h[:, WINDOW : 2 * WINDOW]
            near_r = jnp.where(right_ok, near_h[:, 2 * WINDOW :], masked_value)
            near_max = jnp.maximum(jnp.maximum(near_l, near_m), near_r).max(-1, keepdims=True)
            top = jnp.maximum(
                jnp.maximum(near_max, far_h.max(-1, keepdims=True) + lift), sink
            )
            far_exp = jnp.exp2(far_h - (top - lift)).astype(bf16)
            near_exp = jnp.concatenate(
                [jnp.exp2(part - top).astype(bf16) for part in (near_l, near_m, near_r)], axis=1
            )
            acc = jnp.dot(far_exp, ctx_values, preferred_element_type=f32) + jnp.dot(
                near_exp, near_values, preferred_element_type=f32
            )
            total = pltpu.roll(acc, HEAD, 1) + jnp.exp2(sink - top)
            outs.append(acc / total)
        for pair in range(heads // 2):
            both = jnp.where(lane < HEAD, outs[2 * pair], pltpu.roll(outs[2 * pair + 1], HEAD, 1))
            out_ref[0, sub * WINDOW : (sub + 1) * WINDOW, pair * LANES : (pair + 1) * LANES] = both.astype(bf16)


def attended_rows(place, lift, sink, queries, pairs, left, right, ctx_pieces, sample, tp_count):
    _, tokens, cols = queries.shape
    block = tokens // tp_count
    pieces = len(ctx_pieces)
    piece_rows = ctx_pieces[0].shape[1]
    at_sample = lambda t, *_: (sample, 0, 0)
    whole_of = lambda array: pl.BlockSpec((1,) + array.shape[1:], at_sample)
    keys = pieces * piece_rows
    work = tokens * (keys + 3 * WINDOW) * cols
    grid_spec = pltpu.PrefetchScalarGridSpec(
        num_scalar_prefetch=3,
        grid=(tp_count,),
        in_specs=[pl.BlockSpec((1, block, cols), lambda t, *_: (sample, t, 0))]
        + [whole_of(array) for array in (pairs, left, right, *ctx_pieces)],
        out_specs=pl.BlockSpec(
            (1, block, cols), lambda t, place, *_: (lax.rem(t - place[1] + tp_count, tp_count), 0, 0)
        ),
        scratch_shapes=[
            pltpu.VMEM((tokens + 2 * WINDOW, 2 * HEAD), bf16),
            pltpu.VMEM((tokens + 2 * WINDOW, 2 * HEAD), bf16),
            pltpu.VMEM((keys, 2 * HEAD), bf16),
            pltpu.VMEM((keys, 2 * HEAD), bf16),
        ],
    )
    return pl.pallas_call(
        functools.partial(attend_kernel, pieces=pieces, last_place=lax.axis_size("sp") - 1),
        grid_spec=grid_spec,
        out_shape=jax.ShapeDtypeStruct((tp_count, block, cols), bf16),
        cost_estimate=pl.CostEstimate(flops=4 * work, transcendentals=0, bytes_accessed=work // keys),
        name="attend",
    )(place, lift, sink, queries, pairs, left, right, *ctx_pieces)


def out_kernel(place_ref, *refs, hops):
    gate_ref = refs[0]
    pieces = refs[1 : 1 + hops]
    own_w = refs[1 + hops]
    near_w = refs[2 + hops : 1 + 2 * hops]
    far_w = refs[1 + 2 * hops : 3 * hops]
    out_ref, lhs_scr = refs[-2:]
    first = place_ref[2] == 0

    @pl.when(pl.program_id(0) == 0)
    def _():
        cols = own_w.shape[0]
        lhs_scr[:, :cols] = pieces[0][0]
        for hop in range(1, hops):
            rows = pieces[hop][0]
            half = cols // 2
            low, high = rows[:, :half].astype(f32), rows[:, half:].astype(f32)
            at = hop * cols
            lhs_scr[:, at : at + half] = jnp.where(first, low, high).astype(bf16)
            lhs_scr[:, at + half : at + cols] = jnp.where(first, high, low).astype(bf16)

    blocks = [own_w[...]]
    for hop in range(1, hops):
        blocks += [near_w[hop - 1][...], far_w[hop - 1][...]]
    acc = jnp.dot(lhs_scr[...], jnp.concatenate(blocks, axis=0), preferred_element_type=f32)
    out_ref[0] = (gate_ref[0] * acc).astype(bf16)


def out_rows(place, gate, pieces, own_w, near_w, far_w, sample, samples, previous):
    hops = len(pieces)
    block, cols = pieces[0].shape[1:]
    width = own_w.shape[1]
    tile = min(512, width)
    specs = [pl.BlockSpec((1, 1, tile), lambda n, *_: (sample, 0, n))]
    specs += [pl.BlockSpec((1, block, cols), lambda n, *_: (0, 0, 0))] * hops
    specs += [pl.BlockSpec((cols, tile), lambda n, *_: (0, n))]
    specs += [pl.BlockSpec((cols // 2, tile), lambda n, *_: (0, n))] * (2 * (hops - 1))
    args = [gate, *pieces, own_w, *near_w, *far_w]
    aliases = {}
    if previous is not None:
        specs.append(pl.BlockSpec(memory_space=pl.ANY))
        args.append(previous)
        aliases = {len(args): 0}
    return pl.pallas_call(
        functools.partial(out_kernel, hops=hops),
        grid_spec=pltpu.PrefetchScalarGridSpec(
            num_scalar_prefetch=1,
            grid=(width // tile,),
            in_specs=specs,
            out_specs=pl.BlockSpec((1, block, tile), lambda n, *_: (sample, 0, n)),
            scratch_shapes=[pltpu.VMEM((block, hops * cols), bf16)],
        ),
        out_shape=jax.ShapeDtypeStruct((samples, block, width), bf16),
        input_output_aliases=aliases,
        cost_estimate=pl.CostEstimate(
            flops=2 * block * hops * cols * width, transcendentals=0, bytes_accessed=2 * hops * cols * width
        ),
        name="out_proj",
    )(place, *args)


def shards(
    latent,
    context,
    condition,
    ctx_cond,
    norm_gain,
    w_shift,
    w_scale,
    w_gate,
    w_query,
    w_key,
    w_value,
    w_out,
    sink_logit,
    ctx_lift,
):
    samples, tokens, model_width = latent.shape
    sp_count = lax.axis_size("sp")
    tp_count = lax.axis_size("tp")
    place = jnp.stack(
        [lax.axis_index("sp"), lax.axis_index("tp"), lax.axis_index("dp")]
    ).astype(jnp.int32)
    gain, shift, gate, first_stage = modulation(
        place, condition, ctx_cond, norm_gain, w_shift, w_scale, w_gate
    )
    w_late, offset = lax.optimization_barrier((w_out, place, first_stage))[:2]
    tables = small_tables(tokens, offset[0] * tokens)
    half = w_out.shape[0] // 2
    w_half = lax.dynamic_slice_in_dim(w_late, lax.axis_index("dp") * half, half, 0)
    near_w = [shifted(w_half, "tp", hop) for hop in range(1, tp_count)]
    far_w = [shifted(piece, "dp", 1) for piece in near_w]

    ctx_own, to_next, to_prev = early_pairs(context, latent, gain, shift, w_key, w_value, tables)
    rows = ctx_own.shape[1]
    if 3 <= sp_count <= DIRECT:
        left, right = shifted(to_next, "sp", 1), shifted(to_prev, "sp", sp_count - 1)
        ctx_pieces = [ctx_own, left, right]
        ctx_pieces += [shifted(ctx_own, "sp", hop) for hop in range(2, sp_count - 1)]
    else:
        left = shifted(to_next[:, rows:], "sp", 1)
        right = shifted(to_prev[:, rows:], "sp", sp_count - 1)
        ctx_pieces = [lax.all_gather(ctx_own, "sp", axis=1, tiled=True)]

    queries, pairs = projected_rows(latent, gain, shift, w_query, w_key, w_value, tables)
    arrived = []
    for sample in range(samples):
        attended = attended_rows(
            place, ctx_lift, sink_logit, queries, pairs, left, right, ctx_pieces, sample, tp_count
        )
        arrived.append(
            [attended[:1]] + [shifted(attended[hop : hop + 1], "tp", hop) for hop in range(1, tp_count)]
        )
    mixed = None
    for sample in range(samples):
        mixed = out_rows(place, gate, arrived[sample], w_out, near_w, far_w, sample, samples, mixed)
    return mixed


def solution(mesh):
    return jax.shard_map(
        shards,
        mesh=mesh,
        in_specs=(
            P("dp", "sp", None),
            P("dp", "sp", None),
            P("dp", "sp"),
            P("sp"),
            P(),
            P("sp", "tp"),
            P("sp", "tp"),
            P("sp", "tp"),
            P(None, "tp"),
            P(None, "tp"),
            P(None, "tp"),
            P("tp", None),
            P("tp"),
            P("tp"),
        ),
        out_specs=P("dp", ("sp", "tp"), None),
        check_vma=False,
    )
```

```python
import functools

import jax
import jax.numpy as jnp
from jax import lax
from jax.experimental import pallas as pl
from jax.experimental.pallas import tpu as pltpu
from jax.sharding import PartitionSpec as P

HEAD = 64
WINDOW = 128
GRID_COLS = 64
LANES = 128

epsilon = 1e-06
rope_base = 10000.0
masked_value = -1e30
LOG2E = 1.4426950408889634
DIRECT = 4

f32 = jnp.float32
bf16 = jnp.bfloat16


def shifted(piece, axis, hop):
    count = lax.axis_size(axis)
    return lax.ppermute(piece, axis, [(i, (i + hop) % count) for i in range(count)])


def mod_kernel(cond_ref, ctx_ref, shift_ref, scale_ref, gate_ref, out_ref, rows_scr):
    samples = cond_ref.shape[0]
    rows_scr[:samples] = cond_ref[...].astype(f32)
    rows_scr[samples:] = ctx_ref[...].astype(f32)
    rows = rows_scr[...]
    active = (rows / (1.0 + jnp.exp(-rows))).astype(bf16)
    width = shift_ref.shape[1]
    for slot, weight in enumerate((shift_ref, scale_ref, gate_ref)):
        out_ref[:, slot * width : (slot + 1) * width] = jnp.dot(
            active, weight[...], preferred_element_type=f32
        )


def finish_kernel(place_ref, norm_ref, *refs, hops):
    gain_ref, shift_ref, gate_ref, sum_scr = refs[-4:]
    parts = refs[:-4]
    total = parts[0][...]
    for part in parts[1:]:
        total = total + part[...]
    rows = total.shape[1]
    width = total.shape[2] // 3
    for hop in range(hops):
        owner = lax.rem(place_ref[1] - hop + hops, hops)
        at = pl.ds(pl.multiple_of(owner * width, LANES), width)
        for slot in range(3):
            sum_scr[slot * rows : (slot + 1) * rows, at] = total[hop, :, slot * width : (slot + 1) * width]
    values = sum_scr[...]
    for row in range(rows):
        shift_ref[row] = values[row : row + 1]
        gain_ref[row] = norm_ref[...] * (1.0 + values[rows + row : rows + row + 1])
        gate_ref[row] = values[2 * rows + row : 2 * rows + row + 1]


def modulation(place, condition, ctx_cond, norm_gain, w_shift, w_scale, w_gate):
    rows = condition.shape[0] + 1
    width = w_shift.shape[1]
    part = pl.pallas_call(
        mod_kernel,
        out_shape=jax.ShapeDtypeStruct((rows, 3 * width), f32),
        scratch_shapes=[pltpu.VMEM((rows, condition.shape[1]), f32)],
        name="mod_part",
    )(condition, ctx_cond[None, :], w_shift, w_scale, w_gate)
    sp_count = lax.axis_size("sp")
    tp_count = lax.axis_size("tp")
    gathered = jnp.stack([part] + [shifted(part, "tp", hop) for hop in range(1, tp_count)])
    if sp_count <= DIRECT:
        parts = [gathered] + [shifted(gathered, "sp", hop) for hop in range(1, sp_count)]
    else:
        parts = [lax.psum(gathered, "sp")]
    model_width = norm_gain.shape[0]
    vector = jax.ShapeDtypeStruct((rows, 1, model_width), f32)
    smem = pl.BlockSpec(memory_space=pltpu.SMEM)
    vmem = pl.BlockSpec(memory_space=pltpu.VMEM)
    gain, shift, gate = pl.pallas_call(
        functools.partial(finish_kernel, hops=tp_count),
        in_specs=[smem, vmem] + [vmem] * len(parts),
        out_shape=[vector] * 3,
        scratch_shapes=[pltpu.VMEM((3 * rows, model_width), f32)],
        name="finish",
    )(place, norm_gain[None, :], *parts)
    return gain, shift, gate, gathered


def normed(rows, gain_row, shift_row):
    widened = rows.astype(f32)
    inverse = lax.rsqrt(jnp.mean(widened * widened, axis=-1, keepdims=True) + epsilon)
    return (widened * inverse * gain_row + shift_row).astype(bf16)


def small_tables(tokens, offset):
    quarter = HEAD // 4
    lane = jnp.arange(LANES, dtype=jnp.int32)[None, :]
    frequency = rope_base ** (-(lane % quarter).astype(f32) / quarter)
    groups = tokens // GRID_COLS
    number = jnp.arange(groups + GRID_COLS, dtype=jnp.int32)[:, None]
    of_row = number < groups
    turn = jnp.where(of_row, number + offset // GRID_COLS, number - groups).astype(f32)
    angle = turn * frequency
    used = of_row == (lane % HEAD < HEAD // 2)
    sign = jnp.where(lane // quarter % 2 == 0, -1.0, 1.0)
    return jnp.where(used, jnp.cos(angle), 0.0), jnp.where(used, jnp.sin(angle) * sign, 0.0)


def rotation(cos_ref, sin_ref, group, count):
    groups = cos_ref.shape[0] - GRID_COLS

    def table(ref):
        rows = [ref[pl.ds(group + i, 1), :] + ref[groups:, :] for i in range(count)]
        return jnp.concatenate(rows, axis=0)

    return table(cos_ref), table(sin_ref)


def rotated(part, cosine, sine):
    quarter = HEAD // 4
    lane = lax.broadcasted_iota(jnp.int32, part.shape, 1)
    partner = jnp.where(
        lane // quarter % 2 == 0,
        pltpu.roll(part, LANES - quarter, 1),
        pltpu.roll(part, quarter, 1),
    )
    return part * cosine + partner * sine


def rotated_pairs(part, cosine, sine):
    lane = lax.broadcasted_iota(jnp.int32, part.shape, 1)
    return jnp.where(lane < HEAD, rotated(part, cosine, sine), part).astype(bf16)


def early_kernel(
    x_ref, head_ref, tail_ref, gain_ref, shift_ref, cgain_ref, cshift_ref, wk_ref, wv_ref,
    cos_ref, sin_ref, ctx_ref, next_ref, prev_ref, w_scr,
):
    @pl.when(pl.program_id(0) == 0)
    def _():
        w_scr[:, :HEAD] = wk_ref[...]
        w_scr[:, HEAD:] = wv_ref[...]

    weights = w_scr[...]
    rows = x_ref.shape[1]
    groups = cos_ref.shape[0] - GRID_COLS
    edge = WINDOW // GRID_COLS
    hidden = normed(x_ref[0], cgain_ref[0], cshift_ref[0])
    ctx = jnp.dot(hidden, weights, preferred_element_type=f32).astype(bf16)
    ctx_ref[0] = ctx
    next_ref[0, :rows] = ctx
    prev_ref[0, :rows] = ctx
    for source, target, group in ((head_ref, prev_ref, 0), (tail_ref, next_ref, groups - edge)):
        hidden = normed(source[0], gain_ref[0], shift_ref[0])
        part = jnp.dot(hidden, weights, preferred_element_type=f32)
        target[0, rows:] = rotated_pairs(part, *rotation(cos_ref, sin_ref, group, edge))


def early_pairs(context, latent, gain, shift, w_key, w_value, tables):
    samples, rows, width = context.shape
    last = latent.shape[1] // WINDOW - 1
    vec = pl.BlockSpec((1, 1, width), lambda s: (s, 0, 0))
    ctx_vec = pl.BlockSpec((1, 1, width), lambda s: (samples, 0, 0))
    whole = lambda s: (0, 0)
    sizes = (rows, rows + WINDOW, rows + WINDOW)
    work = samples * (rows + 2 * WINDOW) * width
    return pl.pallas_call(
        early_kernel,
        grid=(samples,),
        in_specs=[
            pl.BlockSpec((1, rows, width), lambda s: (s, 0, 0)),
            pl.BlockSpec((1, WINDOW, width), lambda s: (s, 0, 0)),
            pl.BlockSpec((1, WINDOW, width), lambda s: (s, last, 0)),
            vec,
            vec,
            ctx_vec,
            ctx_vec,
            pl.BlockSpec(w_key.shape, whole),
            pl.BlockSpec(w_value.shape, whole),
            pl.BlockSpec(tables[0].shape, whole),
            pl.BlockSpec(tables[1].shape, whole),
        ],
        out_specs=[pl.BlockSpec((1, size, 2 * HEAD), lambda s: (s, 0, 0)) for size in sizes],
        out_shape=[jax.ShapeDtypeStruct((samples, size, 2 * HEAD), bf16) for size in sizes],
        scratch_shapes=[pltpu.VMEM((width, 2 * HEAD), bf16)],
        cost_estimate=pl.CostEstimate(flops=work * 4 * HEAD, transcendentals=0, bytes_accessed=2 * work),
        name="early_proj",
    )(context, latent, latent, gain, shift, gain, shift, w_key, w_value, *tables)


def proj_kernel(
    x_ref, gain_ref, shift_ref, wq_ref, wk_ref, wv_ref, cos_ref, sin_ref, q_ref, kv_ref, w_scr
):
    cols = wq_ref.shape[1]

    @pl.when((pl.program_id(0) == 0) & (pl.program_id(1) == 0))
    def _():
        w_scr[:, :cols] = wq_ref[...]
        w_scr[:, cols : cols + HEAD] = wk_ref[...]
        w_scr[:, cols + HEAD :] = wv_ref[...]

    count = x_ref.shape[1] // GRID_COLS
    hidden = normed(x_ref[0], gain_ref[0], shift_ref[0])
    product = jnp.dot(hidden, w_scr[...], preferred_element_type=f32)
    cosine, sine = rotation(cos_ref, sin_ref, pl.program_id(1) * count, count)
    for start in range(0, cols, LANES):
        part = rotated(product[:, start : start + LANES], cosine, sine)
        q_ref[0, :, start : start + LANES] = (part * (LOG2E * HEAD**-0.5)).astype(bf16)
    kv_ref[0] = rotated_pairs(product[:, cols:], cosine, sine)


def projected_rows(latent, gain, shift, w_query, w_key, w_value, tables):
    samples, tokens, width = latent.shape
    block = min(256, tokens)
    cols = w_query.shape[1]
    vec = pl.BlockSpec((1, 1, width), lambda s, t: (s, 0, 0))
    whole = lambda s, t: (0, 0)
    work = samples * tokens * width
    return pl.pallas_call(
        proj_kernel,
        grid=(samples, tokens // block),
        in_specs=[
            pl.BlockSpec((1, block, width), lambda s, t: (s, t, 0)),
            vec,
            vec,
            pl.BlockSpec(w_query.shape, whole),
            pl.BlockSpec(w_key.shape, whole),
            pl.BlockSpec(w_value.shape, whole),
            pl.BlockSpec(tables[0].shape, whole),
            pl.BlockSpec(tables[1].shape, whole),
        ],
        out_specs=[
            pl.BlockSpec((1, block, cols), lambda s, t: (s, t, 0)),
            pl.BlockSpec((1, block, 2 * HEAD), lambda s, t: (s, t, 0)),
        ],
        out_shape=[
            jax.ShapeDtypeStruct((samples, tokens, cols), bf16),
            jax.ShapeDtypeStruct((samples, tokens, 2 * HEAD), bf16),
        ],
        scratch_shapes=[pltpu.VMEM((width, cols + 2 * HEAD), bf16)],
        cost_estimate=pl.CostEstimate(
            flops=work * 2 * (cols + 2 * HEAD), transcendentals=0, bytes_accessed=2 * work
        ),
        name="latent_proj",
    )(latent, gain, shift, w_query, w_key, w_value, *tables)


def attend_kernel(place_ref, lift_ref, sink_ref, q_ref, kv_ref, left_ref, right_ref, *rest, pieces, last_place):
    ctx_refs = rest[:pieces]
    out_ref, near_scr, nearv_scr, ctx_scr, ctxv_scr = rest[pieces:]
    step = pl.program_id(0)
    tokens = kv_ref.shape[1]
    piece_rows = ctx_scr.shape[0] // pieces
    block = q_ref.shape[1]
    heads = q_ref.shape[2] // HEAD

    @pl.when(step == 0)
    def _():
        near_scr[:WINDOW] = left_ref[0, left_ref.shape[1] - WINDOW :]
        near_scr[WINDOW : WINDOW + tokens] = kv_ref[0]
        near_scr[WINDOW + tokens :] = right_ref[0, right_ref.shape[1] - WINDOW :]
        for number, ref in enumerate(ctx_refs):
            ctx_scr[number * piece_rows : (number + 1) * piece_rows] = ref[0, :piece_rows]
        for source, target in ((near_scr, nearv_scr), (ctx_scr, ctxv_scr)):
            turned = pltpu.roll(source[...].astype(f32), HEAD, 1)
            lane = lax.broadcasted_iota(jnp.int32, turned.shape, 1)
            target[...] = jnp.where(lane < HEAD, turned, 1.0).astype(bf16)

    ctx_rows, ctx_values = ctx_scr[...], ctxv_scr[...]
    row = lax.broadcasted_iota(jnp.int32, (WINDOW, WINDOW), 0)
    col = lax.broadcasted_iota(jnp.int32, (WINDOW, WINDOW), 1)
    contract = (((1,), (1,)), ((), ()))
    for sub in range(block // WINDOW):
        start = pl.multiple_of(step * block + sub * WINDOW, WINDOW)
        near_rows = near_scr[pl.ds(start, 3 * WINDOW), :]
        near_values = nearv_scr[pl.ds(start, 3 * WINDOW), :]
        left_from = jnp.where((place_ref[0] == 0) & (start == 0), 2 * WINDOW, 0)
        right_from = jnp.where(
            (place_ref[0] == last_place) & (start + WINDOW == tokens), 2 * WINDOW, 0
        )
        left_ok = col >= row + left_from
        right_ok = col + right_from <= row
        stacked = []
        lane = lax.broadcasted_iota(jnp.int32, (WINDOW, LANES), 1)
        for head in range(heads):
            chunk = q_ref[0, sub * WINDOW : (sub + 1) * WINDOW, head // 2 * LANES : head // 2 * LANES + LANES].astype(f32)
            if head % 2:
                chunk = pltpu.roll(chunk, HEAD, 1)
            stacked.append(jnp.where(lane < HEAD, chunk, 0.0).astype(bf16))
        stacked = jnp.concatenate(stacked, axis=0)
        far = lax.dot_general(stacked, ctx_rows, contract, preferred_element_type=f32)
        near = lax.dot_general(stacked, near_rows, contract, preferred_element_type=f32)
        outs = []
        for head in range(heads):
            span = slice(head * WINDOW, (head + 1) * WINDOW)
            lift = lift_ref[head] * LOG2E
            sink = sink_ref[head] * LOG2E
            far_h = far[span]
            near_h = near[span]
            near_l = jnp.where(left_ok, near_h[:, :WINDOW], masked_value)
            near_m = near_h[:, WINDOW : 2 * WINDOW]
            near_r = jnp.where(right_ok, near_h[:, 2 * WINDOW :], masked_value)
            near_max = jnp.maximum(jnp.maximum(near_l, near_m), near_r).max(-1, keepdims=True)
            top = jnp.maximum(
                jnp.maximum(near_max, far_h.max(-1, keepdims=True) + lift), sink
            )
            far_exp = jnp.exp2(far_h - (top - lift)).astype(bf16)
            near_exp = jnp.concatenate(
                [jnp.exp2(part - top).astype(bf16) for part in (near_l, near_m, near_r)], axis=1
            )
            acc = jnp.dot(far_exp, ctx_values, preferred_element_type=f32) + jnp.dot(
                near_exp, near_values, preferred_element_type=f32
            )
            total = pltpu.roll(acc, HEAD, 1) + jnp.exp2(sink - top)
            outs.append(acc / total)
        for pair in range(heads // 2):
            both = jnp.where(lane < HEAD, outs[2 * pair], pltpu.roll(outs[2 * pair + 1], HEAD, 1))
            out_ref[0, sub * WINDOW : (sub + 1) * WINDOW, pair * LANES : (pair + 1) * LANES] = both.astype(bf16)


def attended_rows(place, lift, sink, queries, pairs, left, right, ctx_pieces, sample, tp_count):
    _, tokens, cols = queries.shape
    block = tokens // tp_count
    pieces = len(ctx_pieces)
    piece_rows = ctx_pieces[0].shape[1]
    at_sample = lambda t, *_: (sample, 0, 0)
    whole_of = lambda array: pl.BlockSpec((1,) + array.shape[1:], at_sample)
    keys = pieces * piece_rows
    work = tokens * (keys + 3 * WINDOW) * cols
    grid_spec = pltpu.PrefetchScalarGridSpec(
        num_scalar_prefetch=3,
        grid=(tp_count,),
        in_specs=[pl.BlockSpec((1, block, cols), lambda t, *_: (sample, t, 0))]
        + [whole_of(array) for array in (pairs, left, right, *ctx_pieces)],
        out_specs=pl.BlockSpec(
            (1, block, cols), lambda t, place, *_: (lax.rem(t - place[1] + tp_count, tp_count), 0, 0)
        ),
        scratch_shapes=[
            pltpu.VMEM((tokens + 2 * WINDOW, 2 * HEAD), bf16),
            pltpu.VMEM((tokens + 2 * WINDOW, 2 * HEAD), bf16),
            pltpu.VMEM((keys, 2 * HEAD), bf16),
            pltpu.VMEM((keys, 2 * HEAD), bf16),
        ],
    )
    return pl.pallas_call(
        functools.partial(attend_kernel, pieces=pieces, last_place=lax.axis_size("sp") - 1),
        grid_spec=grid_spec,
        out_shape=jax.ShapeDtypeStruct((tp_count, block, cols), bf16),
        cost_estimate=pl.CostEstimate(flops=4 * work, transcendentals=0, bytes_accessed=work // keys),
        name="attend",
    )(place, lift, sink, queries, pairs, left, right, *ctx_pieces)


def out_kernel(place_ref, gate_ref, *refs, hops, samples):
    pieces = refs[: samples * hops]
    weights = refs[samples * hops : -2]
    out_ref, lhs_scr = refs[-2:]
    first = place_ref[2] == 0
    block = pieces[0].shape[1]

    @pl.when(pl.program_id(0) == 0)
    def _():
        cols = pieces[0].shape[2]
        half = cols // 2
        for sample in range(samples):
            span = slice(sample * block, (sample + 1) * block)
            lhs_scr[span, :cols] = pieces[sample * hops][0]
            for hop in range(1, hops):
                rows = pieces[sample * hops + hop][0]
                low, high = rows[:, :half].astype(f32), rows[:, half:].astype(f32)
                at = hop * cols
                lhs_scr[span, at : at + half] = jnp.where(first, low, high).astype(bf16)
                lhs_scr[span, at + half : at + cols] = jnp.where(first, high, low).astype(bf16)

    joined = jnp.concatenate([weight[...] for weight in weights], axis=0)
    acc = jnp.dot(lhs_scr[...], joined, preferred_element_type=f32)
    for sample in range(samples):
        out_ref[sample] = (gate_ref[sample] * acc[sample * block : (sample + 1) * block]).astype(bf16)


def out_rows(place, gate, arrived, own_w, near_w, far_w):
    samples, hops = len(arrived), len(arrived[0])
    block, cols = arrived[0][0].shape[1:]
    width = own_w.shape[1]
    tile = min(512, width)
    weights = [own_w]
    for near, far in zip(near_w, far_w):
        weights += [near, far]
    pieces = [piece for group in arrived for piece in group]
    specs = [pl.BlockSpec((gate.shape[0], 1, tile), lambda n, *_: (0, 0, n))]
    specs += [pl.BlockSpec((1, block, cols), lambda n, *_: (0, 0, 0))] * len(pieces)
    specs += [pl.BlockSpec((weight.shape[0], tile), lambda n, *_: (0, n)) for weight in weights]
    depth = hops * cols
    return pl.pallas_call(
        functools.partial(out_kernel, hops=hops, samples=samples),
        grid_spec=pltpu.PrefetchScalarGridSpec(
            num_scalar_prefetch=1,
            grid=(width // tile,),
            in_specs=specs,
            out_specs=pl.BlockSpec((samples, block, tile), lambda n, *_: (0, 0, n)),
            scratch_shapes=[pltpu.VMEM((samples * block, depth), bf16)],
        ),
        out_shape=jax.ShapeDtypeStruct((samples, block, width), bf16),
        cost_estimate=pl.CostEstimate(
            flops=2 * samples * block * depth * width, transcendentals=0, bytes_accessed=2 * depth * width
        ),
        name="out_proj",
    )(place, gate, *pieces, *weights)


def shards(
    latent,
    context,
    condition,
    ctx_cond,
    norm_gain,
    w_shift,
    w_scale,
    w_gate,
    w_query,
    w_key,
    w_value,
    w_out,
    sink_logit,
    ctx_lift,
):
    samples, tokens, model_width = latent.shape
    sp_count = lax.axis_size("sp")
    tp_count = lax.axis_size("tp")
    place = jnp.stack(
        [lax.axis_index("sp"), lax.axis_index("tp"), lax.axis_index("dp")]
    ).astype(jnp.int32)
    gain, shift, gate, first_stage = modulation(
        place, condition, ctx_cond, norm_gain, w_shift, w_scale, w_gate
    )
    w_late, offset = lax.optimization_barrier((w_out, place, first_stage))[:2]
    tables = small_tables(tokens, offset[0] * tokens)
    half = w_out.shape[0] // 2
    w_half = lax.dynamic_slice_in_dim(w_late, lax.axis_index("dp") * half, half, 0)
    near_w = [shifted(w_half, "tp", hop) for hop in range(1, tp_count)]
    far_w = [shifted(piece, "dp", 1) for piece in near_w]

    ctx_own, to_next, to_prev = early_pairs(context, latent, gain, shift, w_key, w_value, tables)
    rows = ctx_own.shape[1]
    if 3 <= sp_count <= DIRECT:
        left, right = shifted(to_next, "sp", 1), shifted(to_prev, "sp", sp_count - 1)
        ctx_pieces = [ctx_own, left, right]
        ctx_pieces += [shifted(ctx_own, "sp", hop) for hop in range(2, sp_count - 1)]
    else:
        left = shifted(to_next[:, rows:], "sp", 1)
        right = shifted(to_prev[:, rows:], "sp", sp_count - 1)
        ctx_pieces = [lax.all_gather(ctx_own, "sp", axis=1, tiled=True)]

    queries, pairs = projected_rows(latent, gain, shift, w_query, w_key, w_value, tables)
    arrived = []
    for sample in range(samples):
        attended = attended_rows(
            place, ctx_lift, sink_logit, queries, pairs, left, right, ctx_pieces, sample, tp_count
        )
        arrived.append(
            [attended[:1]] + [shifted(attended[hop : hop + 1], "tp", hop) for hop in range(1, tp_count)]
        )
    return out_rows(place, gate, arrived, w_out, near_w, far_w)


def solution(mesh):
    return jax.shard_map(
        shards,
        mesh=mesh,
        in_specs=(
            P("dp", "sp", None),
            P("dp", "sp", None),
            P("dp", "sp"),
            P("sp"),
            P(),
            P("sp", "tp"),
            P("sp", "tp"),
            P("sp", "tp"),
            P(None, "tp"),
            P(None, "tp"),
            P(None, "tp"),
            P("tp", None),
            P("tp"),
            P("tp"),
        ),
        out_specs=P("dp", ("sp", "tp"), None),
        check_vma=False,
    )
```
